32 devices in a mesh: fs: 16 (over z, y, x), tp: 2 (over core).
Axes of the slice: x: 2, y: 2, z: 4, core: 2. Of those that a mesh axis runs over, the one named last changes fastest.
Arguments:
- prompt: bfloat16 [5120, 2048], P('fs', 'tp'), may hold values from -6 to 6
- norm_gain: float32 [2048], P('fs'), may hold values from 0.1 to 1.9
- gate_master: float32 [2048, 3072], P('fs', 'tp'), may hold values from -0.125 to 0.125
- up_master: float32 [2048, 3072], P('fs', 'tp'), may hold values from -0.125 to 0.125
- down_master: float32 [2048, 3072], P('fs', 'tp'), may hold values from -0.109375 to 0.109375
Outputs:
- gate_new: bfloat16 [3072, 2048], P('tp')
- up_new: bfloat16 [3072, 2048], P('tp')
- down_new: bfloat16 [3072, 2048], P('tp')
- mixed: bfloat16 [2048, 5120], P('tp', 'fs')
The draws below stay inside these ranges and needn't reach their ends.
All inputs are finite; a program needn't handle non-finite values.
Results may differ from the reference program's by a relative error of at most 0.0082.
Values may be sent and summed in bfloat16 or wider, within the bound.
A program may use at most 128 MiB of HBM per device.

```python
import jax
import jax.numpy as jnp
from jax import lax

D = 2048
FF = 3072
TOKENS = 5120


def block_levels(rng, shape, shards, smallest, high):
    factor_of, own = 1.0, jax.random.fold_in(rng, 6)
    for position, parts in shards:
        draws = jnp.exp(jax.random.uniform(jax.random.fold_in(own, position), (parts,), jnp.float32, smallest / len(shards), high / len(shards)))
        factor_of = factor_of * jnp.repeat(draws, shape[position] // parts).reshape([-1 if axis == position else 1 for axis in range(len(shape))])
    return factor_of


def normal_values(rng, extent, spread, limit, pieces=(), dtype=jnp.bfloat16):
    values = spread * jax.random.normal(rng, extent, jnp.float32)
    if pieces:
        values = values * block_levels(rng, extent, pieces, -0.22, 0.18)
    return jnp.clip(values, -limit, limit).astype(dtype)


def setup_inputs(seed: int = 0) -> dict:
    keys = jax.random.split(jax.random.key(seed), 6)
    return {
        "prompt": normal_values(keys[0], (TOKENS, D), 1.0, 6.0, ((0, 16), (1, 2))),
        "norm_gain": jnp.clip(1.0 + 0.18 * jax.random.normal(keys[1], (D,), jnp.float32), 0.1, 1.9),
        "gate_master": normal_values(keys[2], (D, FF), D ** -0.5, 0.125, ((0, 16), (1, 2)), jnp.float32),
        "up_master": normal_values(keys[3], (D, FF), D ** -0.5, 0.125, ((0, 16), (1, 2)), jnp.float32),
        "down_master": normal_values(keys[4], (D, FF), FF ** -0.5, 0.109375, ((0, 16), (1, 2)), jnp.float32),
    }


def reference(prompt, norm_gain, gate_master, up_master, down_master):
    gain_col = norm_gain[:, None]
    gate_new = (gate_master * gain_col).astype(jnp.bfloat16).T
    up_new = (up_master * gain_col).astype(jnp.bfloat16).T
    down_new = down_master.astype(jnp.bfloat16).T
    values = prompt.astype(jnp.float32)
    normed = (values * lax.rsqrt(lax.optimization_barrier(jnp.mean(values * values, axis=1, keepdims=True)) + 1e-06)).astype(jnp.bfloat16)
    gate = jnp.dot(normed, gate_new.T, preferred_element_type=jnp.float32)
    up = jnp.dot(normed, up_new.T, preferred_element_type=jnp.float32)
    hidden = (jax.nn.silu(gate) * up).astype(jnp.bfloat16)
    mixed = jnp.dot(down_new.T, hidden.T, preferred_element_type=jnp.float32).astype(jnp.bfloat16)
    return (gate_new, up_new, down_new, mixed)
```

```python
import functools

import jax
import jax.numpy as jnp
from jax import lax
from jax.experimental import pallas as pl
from jax.experimental.pallas import tpu as pltpu
from jax.sharding import PartitionSpec as P

MESH = pl.DeviceIdType.MESH
LANES = 128
GATE, UP, DOWN = 0, 1, 2
Z_UP, Z_DOWN, ALONG_A, ALONG_B = 0, 1, 2, 3
CHUNKS = 2


def gather_kernel(depth, low_refs, prompt_ref, full_refs, both_ref, send_sem, recv_sem, own_sem, pair_sem):
    fs, tp = lax.axis_index("fs"), lax.axis_index("tp")
    z, y, x = fs // 4, lax.rem(fs // 2, 2), lax.rem(fs, 2)
    at_a, at_b = x * (1 - tp) + y * tp, y * (1 - tp) + x * tp
    to_a, to_b = (1 - 2 * at_a) * (1 + tp), (1 - 2 * at_b) * (2 - tp)
    peers = {Z_UP: fs + 4, Z_DOWN: fs - 4, ALONG_A: fs + to_a, ALONG_B: fs + to_b}
    exists = {Z_UP: z + 1 < depth, Z_DOWN: z > 0, ALONG_A: None, ALONG_B: None}
    rows = low_refs[0].shape[0] // CHUNKS

    def guarded(condition, action):
        if condition is None:
            action()
        else:
            pl.when(condition)(action)

    def both(first, second):
        if first is None:
            return second
        return first if second is None else jnp.logical_and(first, second)

    barrier = pltpu.get_barrier_semaphore()
    pl.semaphore_signal(barrier, inc=1, device_id={"tp": 1 - tp}, device_id_type=MESH)
    for way, peer in peers.items():
        guarded(
            exists[way],
            lambda peer=peer: pl.semaphore_signal(
                barrier, inc=1, device_id={"fs": peer}, device_id_type=MESH
            ),
        )
    along_z = jnp.minimum(z, 1) + jnp.minimum(depth - 1 - z, 1)
    pl.semaphore_wait(barrier, 3 + along_z)

    sent = []

    def copy_of(matrix, way, block, chunk, own):
        part = pl.ds(chunk * rows, rows)
        target = full_refs[matrix].at[block, part]
        return pltpu.make_async_remote_copy(
            src_ref=low_refs[matrix].at[part] if own else target,
            dst_ref=target,
            send_sem=send_sem.at[matrix, way, block, chunk],
            recv_sem=recv_sem.at[matrix, block, chunk],
            device_id={"fs": peers[way]},
            device_id_type=MESH,
        )

    def send(matrix, way, block, chunk, own=False, given=None):
        condition = both(given, exists[way])
        guarded(condition, lambda: copy_of(matrix, way, block, chunk, own).start())
        sent.append((condition, matrix, way, block, chunk, own))

    def arrive(matrix, block, chunk, given=None):
        guarded(given, lambda: copy_of(matrix, ALONG_A, block, chunk, False).wait_recv())

    pair = pltpu.make_async_remote_copy(
        src_ref=prompt_ref,
        dst_ref=both_ref.at[tp],
        send_sem=pair_sem.at[0],
        recv_sem=pair_sem.at[1],
        device_id={"tp": 1 - tp},
        device_id_type=MESH,
    )
    chunks = range(CHUNKS)
    for chunk in chunks:
        send(UP, ALONG_A, fs, chunk, True)
        send(DOWN, ALONG_B, fs, chunk, True)
        send(GATE, Z_UP, fs, chunk, True)
        send(GATE, Z_DOWN, fs, chunk, True)
    for matrix in (UP, DOWN):
        for chunk in chunks:
            send(matrix, Z_UP, fs, chunk, True)
            send(matrix, Z_DOWN, fs, chunk, True)
    for chunk in chunks:
        send(GATE, ALONG_A, fs, chunk, True)
        send(GATE, ALONG_B, fs, chunk, True)
    for chunk in chunks:
        send(DOWN, ALONG_A, fs, chunk, True)
        send(UP, ALONG_B, fs, chunk, True)
    pair.start()
    local = [
        pltpu.make_async_copy(low_refs[m], full_refs[m].at[fs], own_sem.at[m]) for m in (GATE, UP, DOWN)
    ] + [pltpu.make_async_copy(prompt_ref, both_ref.at[tp], own_sem.at[3])]
    for copy in local:
        copy.start()

    for chunk in chunks:
        for matrix, block, last in ((UP, fs + to_a, ALONG_B), (DOWN, fs + to_b, ALONG_A)):
            arrive(matrix, block, chunk)
            send(matrix, Z_UP, block, chunk)
            send(matrix, Z_DOWN, block, chunk)
            send(matrix, last, block, chunk)
    for chunk in chunks:
        arrive(GATE, fs + to_a, chunk)
        send(GATE, ALONG_B, fs + to_a, chunk)
    for step in range(1, depth):
        sides = ((z >= step, fs - 4 * step, Z_UP), (z + step < depth, fs + 4 * step, Z_DOWN))
        for matrix, offset, lasts in (
            (GATE, 0, (ALONG_A, ALONG_B)),
            (UP, 0, (ALONG_B,)),
            (DOWN, 0, (ALONG_A,)),
            (UP, to_a, (ALONG_B,)),
            (DOWN, to_b, (ALONG_A,)),
        ):
            for chunk in chunks:
                for there, block, onward in sides:
                    arrive(matrix, block + offset, chunk, there)
                    if step < depth - 1:
                        send(matrix, onward, block + offset, chunk, given=there)
                    for way in lasts:
                        send(matrix, way, block + offset, chunk, given=there)
        for chunk in chunks:
            for there, block, _ in sides:
                arrive(GATE, block + to_a, chunk, there)
                send(GATE, ALONG_B, block + to_a, chunk, given=there)

    for step in range(depth):
        sides = ((z >= step, fs - 4 * step), (z + step < depth, fs + 4 * step)) if step else ((None, fs),)
        for there, block in sides:
            for chunk in chunks:
                arrive(GATE, block + to_b, chunk, there)
                arrive(GATE, block + to_a + to_b, chunk, there)
                arrive(UP, block + to_b, chunk, there)
                arrive(UP, block + to_a + to_b, chunk, there)
                arrive(DOWN, block + to_a, chunk, there)
                arrive(DOWN, block + to_a + to_b, chunk, there)
    for condition, matrix, way, block, chunk, own in sent:
        guarded(condition, lambda: copy_of(matrix, way, block, chunk, own).wait_send())
    pair.wait()
    for copy in local:
        copy.wait()


def gather(depth, lows, prompt):
    blocks = 4 * depth
    full = jax.ShapeDtypeStruct((blocks,) + lows[0].shape, lows[0].dtype)

    def kernel(g, u, d, p, g_full, u_full, d_full, p_both, *semaphores):
        gather_kernel(depth, (g, u, d), p, (g_full, u_full, d_full), p_both, *semaphores)

    moved = (blocks - 1) * 3 * lows[0].size * 2
    return pl.pallas_call(
        kernel,
        out_shape=(full, full, full, jax.ShapeDtypeStruct((2,) + prompt.shape, prompt.dtype)),
        in_specs=[pl.BlockSpec(memory_space=pltpu.VMEM)] * 4,
        out_specs=[pl.BlockSpec(memory_space=pl.ANY)] * 4,
        scratch_shapes=[
            pltpu.SemaphoreType.DMA((3, 4, blocks, CHUNKS)),
            pltpu.SemaphoreType.DMA((3, blocks, CHUNKS)),
            pltpu.SemaphoreType.DMA((4,)),
            pltpu.SemaphoreType.DMA((2,)),
        ],
        compiler_params=pltpu.CompilerParams(
            collective_id=0, has_side_effects=True
        ),
        cost_estimate=pl.CostEstimate(flops=0, bytes_accessed=2 * moved, transcendentals=0),
        name="gather",
    )(*lows, prompt)


def apply_kernel(steps, both_ref, g_ref, u_ref, d_ref, g_out, u_out, d_out, part_ref, normed, gate, up, hidden):
    k = pl.program_id(0)
    group, rows, lanes = g_ref.shape
    width = group * lanes

    def joined(ref):
        return jnp.concatenate([ref[i] for i in range(group)], axis=1)

    @pl.when(k == 0)
    def _():
        halves = [both_ref[i].astype(jnp.float32) for i in range(both_ref.shape[0])]
        count = sum(half.shape[1] for half in halves)
        total = sum(jnp.sum(half * half, axis=1, keepdims=True) for half in halves)
        scale = lax.rsqrt(total / count + 1e-06)
        values = jnp.concatenate([(half * scale).astype(jnp.bfloat16) for half in halves], axis=1)
        for i in range(steps):
            normed[i] = values[:, i * width : (i + 1) * width]
        gate[...] = jnp.zeros_like(gate)
        up[...] = jnp.zeros_like(up)

    @pl.when(k < steps)
    def _():
        contract = (((1,), (1,)), ((), ()))
        g, u = joined(g_ref), joined(u_ref)
        g_out[...] = g
        u_out[...] = u
        left = normed[k]
        gate[...] += lax.dot_general(left, g, contract, preferred_element_type=jnp.float32)
        up[...] += lax.dot_general(left, u, contract, preferred_element_type=jnp.float32)

    @pl.when(k == steps - 1)
    def _():
        value = gate[...]
        hidden[...] = (value / (1.0 + jnp.exp(-value)) * up[...]).astype(jnp.bfloat16)

    @pl.when(k >= steps)
    def _():
        d = joined(d_ref)
        d_out[...] = d
        part_ref[...] = jnp.dot(hidden[...], d, preferred_element_type=jnp.float32)


def apply(both, g, u, d):
    blocks, rows, lanes = g.shape
    tokens = both.shape[1]
    group = max(n for n in (1, 2, 4) if blocks % n == 0)
    steps, width = blocks // group, group * lanes
    early = lambda k: jnp.minimum(k, steps - 1)
    late = lambda k: jnp.maximum(k - steps, 0)
    whole = jax.ShapeDtypeStruct((rows, blocks * lanes), g.dtype)
    return pl.pallas_call(
        functools.partial(apply_kernel, steps),
        grid=(2 * steps,),
        out_shape=(whole, whole, whole, jax.ShapeDtypeStruct((tokens, blocks * lanes), jnp.float32)),
        in_specs=[
            pl.BlockSpec(both.shape, lambda k: (0, 0, 0)),
            pl.BlockSpec((group, rows, lanes), lambda k: (early(k), 0, 0)),
            pl.BlockSpec((group, rows, lanes), lambda k: (early(k), 0, 0)),
            pl.BlockSpec((group, rows, lanes), lambda k: (late(k), 0, 0)),
        ],
        out_specs=[
            pl.BlockSpec((rows, width), lambda k: (0, early(k))),
            pl.BlockSpec((rows, width), lambda k: (0, early(k))),
            pl.BlockSpec((rows, width), lambda k: (0, late(k))),
            pl.BlockSpec((tokens, width), lambda k: (0, late(k))),
        ],
        scratch_shapes=[
            pltpu.VMEM((steps, tokens, width), jnp.bfloat16),
            pltpu.VMEM((tokens, rows), jnp.float32),
            pltpu.VMEM((tokens, rows), jnp.float32),
            pltpu.VMEM((tokens, rows), jnp.bfloat16),
        ],
        compiler_params=pltpu.CompilerParams(vmem_limit_bytes=56 * 2**20),
        name="apply",
    )(both, g, u, d)


def sum_kernel(part_ref, mixed_ref, other, send_sem, recv_sem):
    tp = lax.axis_index("tp")
    width = other.shape[1]
    barrier = pltpu.get_barrier_semaphore()
    pl.semaphore_signal(barrier, inc=1, device_id={"tp": 1 - tp}, device_id_type=MESH)
    pl.semaphore_wait(barrier, 1)
    copy = pltpu.make_async_remote_copy(
        src_ref=part_ref.at[:, pl.ds(pl.multiple_of((1 - tp) * width, LANES), width)],
        dst_ref=other,
        send_sem=send_sem,
        recv_sem=recv_sem,
        device_id={"tp": 1 - tp},
        device_id_type=MESH,
    )
    copy.start()
    copy.wait()
    own = part_ref[:, pl.ds(pl.multiple_of(tp * width, LANES), width)]
    mixed_ref[...] = (own + other[...]).astype(mixed_ref.dtype)


def summed(part):
    tokens, features = part.shape
    return pl.pallas_call(
        sum_kernel,
        out_shape=jax.ShapeDtypeStruct((tokens, features // 2), jnp.bfloat16),
        in_specs=[pl.BlockSpec(memory_space=pltpu.VMEM)],
        out_specs=pl.BlockSpec(memory_space=pltpu.VMEM),
        scratch_shapes=[
            pltpu.VMEM((tokens, features // 2), jnp.float32),
            pltpu.SemaphoreType.DMA,
            pltpu.SemaphoreType.DMA,
        ],
        compiler_params=pltpu.CompilerParams(collective_id=1, has_side_effects=True),
        name="summed",
    )(part)


def rounded(norm_gain, gate_master, up_master, down_master):
    gain_col = norm_gain[:, None]
    return (
        (gate_master * gain_col).astype(jnp.bfloat16).T,
        (up_master * gain_col).astype(jnp.bfloat16).T,
        down_master.astype(jnp.bfloat16).T,
    )


def by_kernels(depth, prompt, *weights):
    g, u, d, both = gather(depth, rounded(*weights), prompt)
    gate_new, up_new, down_new, part = apply(both, g, u, d)
    return gate_new, up_new, down_new, summed(part).T


def by_collectives(prompt, *weights):
    gate_low, up_low, down_low = rounded(*weights)
    whole = lax.all_gather(prompt, "tp", axis=1, tiled=True)
    values = whole.astype(jnp.float32)
    normed = (values * lax.rsqrt(jnp.mean(values * values, axis=1, keepdims=True) + 1e-06)).astype(
        jnp.bfloat16
    )
    contract = (((1,), (1,)), ((), ()))
    gate_new, up_new, down_new = (
        lax.all_gather(gate_low, "fs", axis=1, tiled=True),
        lax.all_gather(up_low, "fs", axis=1, tiled=True),
        lax.all_gather(down_low, "fs", axis=1, tiled=True),
    )
    gate = lax.dot_general(normed, gate_new, contract, preferred_element_type=jnp.float32)
    up = lax.dot_general(normed, up_new, contract, preferred_element_type=jnp.float32)
    hidden = (jax.nn.silu(gate) * up).astype(jnp.bfloat16)
    mixed = lax.psum_scatter(
        lax.dot_general(
            down_new, hidden, (((0,), (1,)), ((), ())), preferred_element_type=jnp.float32
        ),
        "tp",
        scatter_dimension=0,
        tiled=True,
    )
    return (gate_new, up_new, down_new, mixed.astype(jnp.bfloat16))


def solution(mesh):
    placed = (P("fs", "tp"), P("fs"), P("fs", "tp"), P("fs", "tp"), P("fs", "tp"))
    members, pair = mesh.shape["fs"], mesh.shape["tp"]

    def on_device(prompt, norm_gain, *masters):
        aligned = norm_gain.shape[0] % LANES == 0 and masters[0].shape[1] % (16 * CHUNKS) == 0
        if aligned and pair == 2 and members % 4 == 0 and prompt.shape[0] % 16 == 0:
            return by_kernels(members // 4, prompt, norm_gain, *masters)
        return by_collectives(prompt, norm_gain, *masters)

    return jax.shard_map(
        on_device,
        mesh=mesh,
        in_specs=placed,
        out_specs=(P("tp", None), P("tp", None), P("tp", None), P("tp", "fs")),
        check_vma=False,
    )
```

```python
import functools

import jax
import jax.numpy as jnp
from jax import lax
from jax.experimental import pallas as pl
from jax.experimental.pallas import tpu as pltpu
from jax.sharding import PartitionSpec as P

MESH = pl.DeviceIdType.MESH
LANES = 128
GATE, UP, DOWN = 0, 1, 2
Z_UP, Z_DOWN, ALONG_A, ALONG_B = 0, 1, 2, 3
CHUNKS = 2


def gather_kernel(depth, low_refs, prompt_ref, full_refs, both_ref, send_sem, recv_sem, pair_sem):
    fs, tp = lax.axis_index("fs"), lax.axis_index("tp")
    z, y, x = fs // 4, lax.rem(fs // 2, 2), lax.rem(fs, 2)
    at_a, at_b = x * (1 - tp) + y * tp, y * (1 - tp) + x * tp
    to_a, to_b = (1 - 2 * at_a) * (1 + tp), (1 - 2 * at_b) * (2 - tp)
    peers = {Z_UP: fs + 4, Z_DOWN: fs - 4, ALONG_A: fs + to_a, ALONG_B: fs + to_b}
    exists = {Z_UP: z + 1 < depth, Z_DOWN: z > 0, ALONG_A: None, ALONG_B: None}
    rows = low_refs[0].shape[0] // CHUNKS

    def guarded(condition, action):
        if condition is None:
            action()
        else:
            pl.when(condition)(action)

    def both(first, second):
        if first is None:
            return second
        return first if second is None else jnp.logical_and(first, second)

    barrier = pltpu.get_barrier_semaphore()
    pl.semaphore_signal(barrier, inc=1, device_id={"tp": 1 - tp}, device_id_type=MESH)
    for way, peer in peers.items():
        guarded(
            exists[way],
            lambda peer=peer: pl.semaphore_signal(
                barrier, inc=1, device_id={"fs": peer}, device_id_type=MESH
            ),
        )
    along_z = jnp.minimum(z, 1) + jnp.minimum(depth - 1 - z, 1)
    pl.semaphore_wait(barrier, 3 + along_z)

    sent = []

    def copy_of(matrix, way, block, chunk, own):
        part = pl.ds(chunk * rows, rows)
        target = full_refs[matrix].at[block, part]
        return pltpu.make_async_remote_copy(
            src_ref=low_refs[matrix].at[part] if own else target,
            dst_ref=target,
            send_sem=send_sem.at[matrix, way, block, chunk],
            recv_sem=recv_sem.at[matrix, block, chunk],
            device_id={"fs": peers[way]},
            device_id_type=MESH,
        )

    def send(matrix, way, block, chunk, own=False, given=None):
        condition = both(given, exists[way])
        guarded(condition, lambda: copy_of(matrix, way, block, chunk, own).start())
        sent.append((condition, matrix, way, block, chunk, own))

    def arrive(matrix, block, chunk, given=None):
        guarded(given, lambda: copy_of(matrix, ALONG_A, block, chunk, False).wait_recv())

    pair = pltpu.make_async_remote_copy(
        src_ref=prompt_ref,
        dst_ref=both_ref.at[tp],
        send_sem=pair_sem.at[0],
        recv_sem=pair_sem.at[1],
        device_id={"tp": 1 - tp},
        device_id_type=MESH,
    )
    chunks = range(CHUNKS)
    for chunk in chunks:
        send(UP, ALONG_A, fs, chunk, True)
        send(DOWN, ALONG_B, fs, chunk, True)
        send(GATE, Z_UP, fs, chunk, True)
        send(GATE, Z_DOWN, fs, chunk, True)
    for matrix in (UP, DOWN):
        for chunk in chunks:
            send(matrix, Z_UP, fs, chunk, True)
            send(matrix, Z_DOWN, fs, chunk, True)
    for chunk in chunks:
        send(GATE, ALONG_A, fs, chunk, True)
        send(GATE, ALONG_B, fs, chunk, True)
    for chunk in chunks:
        send(DOWN, ALONG_A, fs, chunk, True)
        send(UP, ALONG_B, fs, chunk, True)
    pair.start()
    for low, full in zip(low_refs, full_refs):
        full[fs] = low[...]
    both_ref[tp] = prompt_ref[...]

    for chunk in chunks:
        for matrix, block, last in ((UP, fs + to_a, ALONG_B), (DOWN, fs + to_b, ALONG_A)):
            arrive(matrix, block, chunk)
            send(matrix, Z_UP, block, chunk)
            send(matrix, Z_DOWN, block, chunk)
            send(matrix, last, block, chunk)
    for chunk in chunks:
        arrive(GATE, fs + to_a, chunk)
        send(GATE, ALONG_B, fs + to_a, chunk)
    for step in range(1, depth):
        sides = ((z >= step, fs - 4 * step, Z_UP), (z + step < depth, fs + 4 * step, Z_DOWN))
        for matrix, offset, lasts in (
            (GATE, 0, (ALONG_A, ALONG_B)),
            (UP, 0, (ALONG_B,)),
            (DOWN, 0, (ALONG_A,)),
            (UP, to_a, (ALONG_B,)),
            (DOWN, to_b, (ALONG_A,)),
        ):
            for chunk in chunks:
                for there, block, onward in sides:
                    arrive(matrix, block + offset, chunk, there)
                    if step < depth - 1:
                        send(matrix, onward, block + offset, chunk, given=there)
                    for way in lasts:
                        send(matrix, way, block + offset, chunk, given=there)
        for chunk in chunks:
            for there, block, _ in sides:
                arrive(GATE, block + to_a, chunk, there)
                send(GATE, ALONG_B, block + to_a, chunk, given=there)

    for step in range(depth):
        sides = ((z >= step, fs - 4 * step), (z + step < depth, fs + 4 * step)) if step else ((None, fs),)
        for there, block in sides:
            for chunk in chunks:
                arrive(GATE, block + to_b, chunk, there)
                arrive(GATE, block + to_a + to_b, chunk, there)
                arrive(UP, block + to_b, chunk, there)
                arrive(UP, block + to_a + to_b, chunk, there)
                arrive(DOWN, block + to_a, chunk, there)
                arrive(DOWN, block + to_a + to_b, chunk, there)
    for condition, matrix, way, block, chunk, own in sent:
        guarded(condition, lambda: copy_of(matrix, way, block, chunk, own).wait_send())
    pair.wait()


def gather(depth, lows, prompt):
    blocks = 4 * depth
    full = pltpu.VMEM((blocks,) + lows[0].shape, lows[0].dtype)

    def kernel(g, u, d, p, g_full, u_full, d_full, p_both, *semaphores):
        gather_kernel(depth, (g, u, d), p, (g_full, u_full, d_full), p_both, *semaphores)

    moved = (blocks - 1) * 3 * lows[0].size * 2
    return pl.pallas_call(
        kernel,
        out_shape=(full, full, full, pltpu.VMEM((2,) + prompt.shape, prompt.dtype)),
        in_specs=[pl.BlockSpec(memory_space=pltpu.VMEM)] * 4,
        out_specs=[pl.BlockSpec(memory_space=pltpu.VMEM)] * 4,
        scratch_shapes=[
            pltpu.SemaphoreType.DMA((3, 4, blocks, CHUNKS)),
            pltpu.SemaphoreType.DMA((3, blocks, CHUNKS)),
            pltpu.SemaphoreType.DMA((2,)),
        ],
        compiler_params=pltpu.CompilerParams(
            collective_id=0, has_side_effects=True, vmem_limit_bytes=26 * 2**20
        ),
        cost_estimate=pl.CostEstimate(flops=0, bytes_accessed=2 * moved, transcendentals=0),
        name="gather",
    )(*lows, prompt)


def apply_kernel(steps, both_ref, g_ref, u_ref, d_ref, g_out, u_out, d_out, part_ref, normed, gate, up, hidden):
    k = pl.program_id(0)
    group = g_ref.shape[0] // steps
    width = group * g_ref.shape[2]

    def joined(ref, first):
        return jnp.concatenate([ref[first * group + i] for i in range(group)], axis=1)

    @pl.when(k == 0)
    def _():
        halves = [both_ref[i].astype(jnp.float32) for i in range(both_ref.shape[0])]
        count = sum(half.shape[1] for half in halves)
        total = sum(jnp.sum(half * half, axis=1, keepdims=True) for half in halves)
        scale = lax.rsqrt(total / count + 1e-06)
        values = jnp.concatenate([(half * scale).astype(jnp.bfloat16) for half in halves], axis=1)
        for i in range(steps):
            normed[i] = values[:, i * width : (i + 1) * width]
        gate[...] = jnp.zeros_like(gate)
        up[...] = jnp.zeros_like(up)

    @pl.when(k < steps)
    def _():
        contract = (((1,), (1,)), ((), ()))
        g, u = joined(g_ref, k), joined(u_ref, k)
        g_out[...] = g
        u_out[...] = u
        left = normed[k]
        gate[...] += lax.dot_general(left, g, contract, preferred_element_type=jnp.float32)
        up[...] += lax.dot_general(left, u, contract, preferred_element_type=jnp.float32)

    @pl.when(k == steps - 1)
    def _():
        value = gate[...]
        hidden[...] = (value / (1.0 + jnp.exp(-value)) * up[...]).astype(jnp.bfloat16)

    @pl.when(k >= steps)
    def _():
        d = joined(d_ref, k - steps)
        d_out[...] = d
        part_ref[...] = jnp.dot(hidden[...], d, preferred_element_type=jnp.float32)


def apply(both, g, u, d):
    blocks, rows, lanes = g.shape
    tokens = both.shape[1]
    group = max(n for n in (1, 2, 4) if blocks % n == 0)
    steps, width = blocks // group, group * lanes
    early = lambda k: jnp.minimum(k, steps - 1)
    late = lambda k: jnp.maximum(k - steps, 0)
    whole = jax.ShapeDtypeStruct((rows, blocks * lanes), g.dtype)
    return pl.pallas_call(
        functools.partial(apply_kernel, steps),
        grid=(2 * steps,),
        out_shape=(whole, whole, whole, jax.ShapeDtypeStruct((tokens, blocks * lanes), jnp.float32)),
        in_specs=[
            pl.BlockSpec(memory_space=pltpu.VMEM),
            pl.BlockSpec(memory_space=pltpu.VMEM),
            pl.BlockSpec(memory_space=pltpu.VMEM),
            pl.BlockSpec(memory_space=pltpu.VMEM),
        ],
        out_specs=[
            pl.BlockSpec((rows, width), lambda k: (0, early(k))),
            pl.BlockSpec((rows, width), lambda k: (0, early(k))),
            pl.BlockSpec((rows, width), lambda k: (0, late(k))),
            pl.BlockSpec((tokens, width), lambda k: (0, late(k))),
        ],
        scratch_shapes=[
            pltpu.VMEM((steps, tokens, width), jnp.bfloat16),
            pltpu.VMEM((tokens, rows), jnp.float32),
            pltpu.VMEM((tokens, rows), jnp.float32),
            pltpu.VMEM((tokens, rows), jnp.bfloat16),
        ],
        compiler_params=pltpu.CompilerParams(vmem_limit_bytes=32 * 2**20),
        name="apply",
    )(both, g, u, d)


def sum_kernel(part_ref, mixed_ref, other, send_sem, recv_sem):
    tp = lax.axis_index("tp")
    width = other.shape[1]
    barrier = pltpu.get_barrier_semaphore()
    pl.semaphore_signal(barrier, inc=1, device_id={"tp": 1 - tp}, device_id_type=MESH)
    pl.semaphore_wait(barrier, 1)
    copy = pltpu.make_async_remote_copy(
        src_ref=part_ref.at[:, pl.ds(pl.multiple_of((1 - tp) * width, LANES), width)],
        dst_ref=other,
        send_sem=send_sem,
        recv_sem=recv_sem,
        device_id={"tp": 1 - tp},
        device_id_type=MESH,
    )
    copy.start()
    copy.wait()
    own = part_ref[:, pl.ds(pl.multiple_of(tp * width, LANES), width)]
    mixed_ref[...] = (own + other[...]).astype(mixed_ref.dtype)


def summed(part):
    tokens, features = part.shape
    return pl.pallas_call(
        sum_kernel,
        out_shape=jax.ShapeDtypeStruct((tokens, features // 2), jnp.bfloat16),
        in_specs=[pl.BlockSpec(memory_space=pltpu.VMEM)],
        out_specs=pl.BlockSpec(memory_space=pltpu.VMEM),
        scratch_shapes=[
            pltpu.VMEM((tokens, features // 2), jnp.float32),
            pltpu.SemaphoreType.DMA,
            pltpu.SemaphoreType.DMA,
        ],
        compiler_params=pltpu.CompilerParams(collective_id=1, has_side_effects=True, vmem_limit_bytes=12 * 2**20),
        name="summed",
    )(part)


def rounded(norm_gain, gate_master, up_master, down_master):
    gain_col = norm_gain[:, None]
    return (
        (gate_master * gain_col).astype(jnp.bfloat16).T,
        (up_master * gain_col).astype(jnp.bfloat16).T,
        down_master.astype(jnp.bfloat16).T,
    )


def round_kernel(gain_ref, g_ref, u_ref, d_ref, g_out, u_out, d_out):
    gain = gain_ref[...]
    g_out[...] = (g_ref[...] * gain).T.astype(g_out.dtype)
    u_out[...] = (u_ref[...] * gain).T.astype(u_out.dtype)
    d_out[...] = d_ref[...].T.astype(d_out.dtype)


def rounded_by_kernel(norm_gain, *masters):
    features, rows = masters[0].shape
    width = max(n for n in (LANES, 2 * LANES, 4 * LANES) if rows % n == 0)
    low = jax.ShapeDtypeStruct((rows, features), jnp.bfloat16)
    return pl.pallas_call(
        round_kernel,
        grid=(rows // width,),
        out_shape=(low,) * 3,
        in_specs=[pl.BlockSpec((features, 1), lambda k: (0, 0))]
        + [pl.BlockSpec((features, width), lambda k: (0, k))] * 3,
        out_specs=[pl.BlockSpec((width, features), lambda k: (k, 0))] * 3,
        compiler_params=pltpu.CompilerParams(vmem_limit_bytes=8 * 2**20),
        name="rounded",
    )(norm_gain[:, None], *masters)


def by_kernels(depth, prompt, *weights):
    g, u, d, both = gather(depth, rounded_by_kernel(*weights), prompt)
    gate_new, up_new, down_new, part = apply(both, g, u, d)
    return gate_new, up_new, down_new, summed(part).T


def by_collectives(prompt, *weights):
    gate_low, up_low, down_low = rounded(*weights)
    whole = lax.all_gather(prompt, "tp", axis=1, tiled=True)
    values = whole.astype(jnp.float32)
    normed = (values * lax.rsqrt(jnp.mean(values * values, axis=1, keepdims=True) + 1e-06)).astype(
        jnp.bfloat16
    )
    contract = (((1,), (1,)), ((), ()))
    gate_new, up_new, down_new = (
        lax.all_gather(gate_low, "fs", axis=1, tiled=True),
        lax.all_gather(up_low, "fs", axis=1, tiled=True),
        lax.all_gather(down_low, "fs", axis=1, tiled=True),
    )
    gate = lax.dot_general(normed, gate_new, contract, preferred_element_type=jnp.float32)
    up = lax.dot_general(normed, up_new, contract, preferred_element_type=jnp.float32)
    hidden = (jax.nn.silu(gate) * up).astype(jnp.bfloat16)
    mixed = lax.psum_scatter(
        lax.dot_general(
            down_new, hidden, (((0,), (1,)), ((), ())), preferred_element_type=jnp.float32
        ),
        "tp",
        scatter_dimension=0,
        tiled=True,
    )
    return (gate_new, up_new, down_new, mixed.astype(jnp.bfloat16))


def solution(mesh):
    placed = (P("fs", "tp"), P("fs"), P("fs", "tp"), P("fs", "tp"), P("fs", "tp"))
    members, pair = mesh.shape["fs"], mesh.shape["tp"]

    def on_device(prompt, norm_gain, *masters):
        aligned = norm_gain.shape[0] % LANES == 0 and masters[0].shape[1] % LANES == 0
        if aligned and pair == 2 and members % 4 == 0 and prompt.shape[0] % 16 == 0:
            return by_kernels(members // 4, prompt, norm_gain, *masters)
        return by_collectives(prompt, norm_gain, *masters)

    return jax.shard_map(
        on_device,
        mesh=mesh,
        in_specs=placed,
        out_specs=(P("tp", None), P("tp", None), P("tp", None), P("tp", "fs")),
        check_vma=False,
    )
```

```python
import functools

import jax
import jax.numpy as jnp
from jax import lax
from jax.experimental import pallas as pl
from jax.experimental.pallas import tpu as pltpu
from jax.sharding import PartitionSpec as P

MESH = pl.DeviceIdType.MESH
LANES = 128
GATE, UP, DOWN = 0, 1, 2
Z_UP, Z_DOWN, ALONG_A, ALONG_B = 0, 1, 2, 3
CHUNKS = 4


def gather_kernel(depth, low_refs, prompt_ref, full_refs, both_ref, send_sem, recv_sem, pair_sem):
    fs, tp = lax.axis_index("fs"), lax.axis_index("tp")
    z, y, x = fs // 4, lax.rem(fs // 2, 2), lax.rem(fs, 2)
    at_a, at_b = x * (1 - tp) + y * tp, y * (1 - tp) + x * tp
    to_a, to_b = (1 - 2 * at_a) * (1 + tp), (1 - 2 * at_b) * (2 - tp)
    peers = {Z_UP: fs + 4, Z_DOWN: fs - 4, ALONG_A: fs + to_a, ALONG_B: fs + to_b}
    exists = {Z_UP: z + 1 < depth, Z_DOWN: z > 0, ALONG_A: None, ALONG_B: None}
    rows = low_refs[0].shape[0] // CHUNKS

    def guarded(condition, action):
        if condition is None:
            action()
        else:
            pl.when(condition)(action)

    def both(first, second):
        if first is None:
            return second
        return first if second is None else jnp.logical_and(first, second)

    barrier = pltpu.get_barrier_semaphore()
    pl.semaphore_signal(barrier, inc=1, device_id={"tp": 1 - tp}, device_id_type=MESH)
    for way, peer in peers.items():
        guarded(
            exists[way],
            lambda peer=peer: pl.semaphore_signal(
                barrier, inc=1, device_id={"fs": peer}, device_id_type=MESH
            ),
        )
    along_z = jnp.minimum(z, 1) + jnp.minimum(depth - 1 - z, 1)
    pl.semaphore_wait(barrier, 3 + along_z)

    sent = []

    def copy_of(matrix, way, block, chunk, own):
        part = pl.ds(chunk * rows, rows)
        target = full_refs[matrix].at[block, part]
        return pltpu.make_async_remote_copy(
            src_ref=low_refs[matrix].at[part] if own else target,
            dst_ref=target,
            send_sem=send_sem.at[matrix, way, block, chunk],
            recv_sem=recv_sem.at[matrix, block, chunk],
            device_id={"fs": peers[way]},
            device_id_type=MESH,
        )

    def send(matrix, way, block, chunk, own=False, given=None):
        condition = both(given, exists[way])
        guarded(condition, lambda: copy_of(matrix, way, block, chunk, own).start())
        sent.append((condition, matrix, way, block, chunk, own))

    def arrive(matrix, block, chunk, given=None):
        guarded(given, lambda: copy_of(matrix, ALONG_A, block, chunk, False).wait_recv())

    pair = pltpu.make_async_remote_copy(
        src_ref=prompt_ref,
        dst_ref=both_ref.at[tp],
        send_sem=pair_sem.at[0],
        recv_sem=pair_sem.at[1],
        device_id={"tp": 1 - tp},
        device_id_type=MESH,
    )
    chunks = range(CHUNKS)
    for chunk in chunks:
        send(UP, ALONG_A, fs, chunk, True)
        send(DOWN, ALONG_B, fs, chunk, True)
        send(GATE, Z_UP, fs, chunk, True)
        send(GATE, Z_DOWN, fs, chunk, True)
    for matrix in (UP, DOWN):
        for chunk in chunks:
            send(matrix, Z_UP, fs, chunk, True)
            send(matrix, Z_DOWN, fs, chunk, True)
    for chunk in chunks:
        send(GATE, ALONG_A, fs, chunk, True)
        send(GATE, ALONG_B, fs, chunk, True)
    for chunk in chunks:
        send(DOWN, ALONG_A, fs, chunk, True)
        send(UP, ALONG_B, fs, chunk, True)
    pair.start()
    for low, full in zip(low_refs, full_refs):
        full[fs] = low[...]
    both_ref[tp] = prompt_ref[...]

    for chunk in chunks:
        for matrix, block, last in ((UP, fs + to_a, ALONG_B), (DOWN, fs + to_b, ALONG_A)):
            arrive(matrix, block, chunk)
            send(matrix, Z_UP, block, chunk)
            send(matrix, Z_DOWN, block, chunk)
            send(matrix, last, block, chunk)
    for chunk in chunks:
        arrive(GATE, fs + to_a, chunk)
        send(GATE, ALONG_B, fs + to_a, chunk)
    for step in range(1, depth):
        sides = ((z >= step, fs - 4 * step, Z_UP), (z + step < depth, fs + 4 * step, Z_DOWN))
        for matrix, offset, lasts in (
            (GATE, 0, (ALONG_A, ALONG_B)),
            (UP, 0, (ALONG_B,)),
            (DOWN, 0, (ALONG_A,)),
            (UP, to_a, (ALONG_B,)),
            (DOWN, to_b, (ALONG_A,)),
        ):
            for chunk in chunks:
                for there, block, onward in sides:
                    arrive(matrix, block + offset, chunk, there)
                    if step < depth - 1:
                        send(matrix, onward, block + offset, chunk, given=there)
                    for way in lasts:
                        send(matrix, way, block + offset, chunk, given=there)
        for chunk in chunks:
            for there, block, _ in sides:
                arrive(GATE, block + to_a, chunk, there)
                send(GATE, ALONG_B, block + to_a, chunk, given=there)

    for step in range(depth):
        sides = ((z >= step, fs - 4 * step), (z + step < depth, fs + 4 * step)) if step else ((None, fs),)
        for there, block in sides:
            for chunk in chunks:
                arrive(GATE, block + to_b, chunk, there)
                arrive(GATE, block + to_a + to_b, chunk, there)
                arrive(UP, block + to_b, chunk, there)
                arrive(UP, block + to_a + to_b, chunk, there)
                arrive(DOWN, block + to_a, chunk, there)
                arrive(DOWN, block + to_a + to_b, chunk, there)
    for condition, matrix, way, block, chunk, own in sent:
        guarded(condition, lambda: copy_of(matrix, way, block, chunk, own).wait_send())
    pair.wait()


def gather(depth, lows, prompt):
    blocks = 4 * depth
    full = pltpu.VMEM((blocks,) + lows[0].shape, lows[0].dtype)

    def kernel(g, u, d, p, g_full, u_full, d_full, p_both, *semaphores):
        gather_kernel(depth, (g, u, d), p, (g_full, u_full, d_full), p_both, *semaphores)

    moved = (blocks - 1) * 3 * lows[0].size * 2
    return pl.pallas_call(
        kernel,
        out_shape=(full, full, full, pltpu.VMEM((2,) + prompt.shape, prompt.dtype)),
        in_specs=[pl.BlockSpec(memory_space=pltpu.VMEM)] * 4,
        out_specs=[pl.BlockSpec(memory_space=pltpu.VMEM)] * 4,
        scratch_shapes=[
            pltpu.SemaphoreType.DMA((3, 4, blocks, CHUNKS)),
            pltpu.SemaphoreType.DMA((3, blocks, CHUNKS)),
            pltpu.SemaphoreType.DMA((2,)),
        ],
        compiler_params=pltpu.CompilerParams(
            collective_id=0, has_side_effects=True, vmem_limit_bytes=26 * 2**20
        ),
        cost_estimate=pl.CostEstimate(flops=0, bytes_accessed=2 * moved, transcendentals=0),
        name="gather",
    )(*lows, prompt)


def apply_kernel(steps, both_ref, g_ref, u_ref, d_ref, g_out, u_out, d_out, part_ref, normed, gate, up, hidden):
    k = pl.program_id(0)
    group = g_ref.shape[0] // steps
    width = group * g_ref.shape[2]

    def joined(ref, first):
        return jnp.concatenate([ref[first * group + i] for i in range(group)], axis=1)

    @pl.when(k == 0)
    def _():
        halves = [both_ref[i].astype(jnp.float32) for i in range(both_ref.shape[0])]
        count = sum(half.shape[1] for half in halves)
        total = sum(jnp.sum(half * half, axis=1, keepdims=True) for half in halves)
        scale = lax.rsqrt(total / count + 1e-06)
        values = jnp.concatenate([(half * scale).astype(jnp.bfloat16) for half in halves], axis=1)
        for i in range(steps):
            normed[i] = values[:, i * width : (i + 1) * width]
        gate[...] = jnp.zeros_like(gate)
        up[...] = jnp.zeros_like(up)

    @pl.when(k < steps)
    def _():
        contract = (((1,), (1,)), ((), ()))
        g, u = joined(g_ref, k), joined(u_ref, k)
        g_out[...] = g
        u_out[...] = u
        left = normed[k]
        gate[...] += lax.dot_general(left, g, contract, preferred_element_type=jnp.float32)
        up[...] += lax.dot_general(left, u, contract, preferred_element_type=jnp.float32)

    @pl.when(k == steps - 1)
    def _():
        value = gate[...]
        hidden[...] = (value / (1.0 + jnp.exp(-value)) * up[...]).astype(jnp.bfloat16)

    @pl.when(k >= steps)
    def _():
        d = joined(d_ref, k - steps)
        d_out[...] = d
        part_ref[...] = jnp.dot(hidden[...], d, preferred_element_type=jnp.float32)


def apply(both, g, u, d):
    blocks, rows, lanes = g.shape
    tokens = both.shape[1]
    group = max(n for n in (1, 2, 4) if blocks % n == 0)
    steps, width = blocks // group, group * lanes
    early = lambda k: jnp.minimum(k, steps - 1)
    late = lambda k: jnp.maximum(k - steps, 0)
    whole = jax.ShapeDtypeStruct((rows, blocks * lanes), g.dtype)
    return pl.pallas_call(
        functools.partial(apply_kernel, steps),
        grid=(2 * steps,),
        out_shape=(whole, whole, whole, jax.ShapeDtypeStruct((tokens, blocks * lanes), jnp.float32)),
        in_specs=[
            pl.BlockSpec(memory_space=pltpu.VMEM),
            pl.BlockSpec(memory_space=pltpu.VMEM),
            pl.BlockSpec(memory_space=pltpu.VMEM),
            pl.BlockSpec(memory_space=pltpu.VMEM),
        ],
        out_specs=[
            pl.BlockSpec((rows, width), lambda k: (0, early(k))),
            pl.BlockSpec((rows, width), lambda k: (0, early(k))),
            pl.BlockSpec((rows, width), lambda k: (0, late(k))),
            pl.BlockSpec((tokens, width), lambda k: (0, late(k))),
        ],
        scratch_shapes=[
            pltpu.VMEM((steps, tokens, width), jnp.bfloat16),
            pltpu.VMEM((tokens, rows), jnp.float32),
            pltpu.VMEM((tokens, rows), jnp.float32),
            pltpu.VMEM((tokens, rows), jnp.bfloat16),
        ],
        compiler_params=pltpu.CompilerParams(vmem_limit_bytes=32 * 2**20),
        name="apply",
    )(both, g, u, d)


def sum_kernel(part_ref, mixed_ref, other, send_sem, recv_sem):
    tp = lax.axis_index("tp")
    width = other.shape[1]
    barrier = pltpu.get_barrier_semaphore()
    pl.semaphore_signal(barrier, inc=1, device_id={"tp": 1 - tp}, device_id_type=MESH)
    pl.semaphore_wait(barrier, 1)
    copy = pltpu.make_async_remote_copy(
        src_ref=part_ref.at[:, pl.ds(pl.multiple_of((1 - tp) * width, LANES), width)],
        dst_ref=other,
        send_sem=send_sem,
        recv_sem=recv_sem,
        device_id={"tp": 1 - tp},
        device_id_type=MESH,
    )
    copy.start()
    copy.wait()
    own = part_ref[:, pl.ds(pl.multiple_of(tp * width, LANES), width)]
    mixed_ref[...] = (own + other[...]).astype(mixed_ref.dtype)


def summed(part):
    tokens, features = part.shape
    return pl.pallas_call(
        sum_kernel,
        out_shape=jax.ShapeDtypeStruct((tokens, features // 2), jnp.bfloat16),
        in_specs=[pl.BlockSpec(memory_space=pltpu.VMEM)],
        out_specs=pl.BlockSpec(memory_space=pltpu.VMEM),
        scratch_shapes=[
            pltpu.VMEM((tokens, features // 2), jnp.float32),
            pltpu.SemaphoreType.DMA,
            pltpu.SemaphoreType.DMA,
        ],
        compiler_params=pltpu.CompilerParams(collective_id=1, has_side_effects=True, vmem_limit_bytes=12 * 2**20),
        name="summed",
    )(part)


def rounded(norm_gain, gate_master, up_master, down_master):
    gain_col = norm_gain[:, None]
    return (
        (gate_master * gain_col).astype(jnp.bfloat16).T,
        (up_master * gain_col).astype(jnp.bfloat16).T,
        down_master.astype(jnp.bfloat16).T,
    )


def round_kernel(gain_ref, g_ref, u_ref, d_ref, g_out, u_out, d_out, held, sems):
    copies = [
        pltpu.make_async_copy(ref, held.at[i], sems.at[i]) for i, ref in enumerate((g_ref, u_ref, d_ref))
    ]
    for copy in copies:
        copy.start()
    gain = gain_ref[...]
    copies[0].wait()
    g_out[...] = (held[0].T * gain).astype(g_out.dtype)
    copies[1].wait()
    u_out[...] = (held[1].T * gain).astype(u_out.dtype)
    copies[2].wait()
    d_out[...] = held[2].T.astype(d_out.dtype)


def rounded_by_kernel(norm_gain, *masters):
    features, rows = masters[0].shape
    low = pltpu.VMEM((rows, features), jnp.bfloat16)
    return pl.pallas_call(
        round_kernel,
        out_shape=(low,) * 3,
        in_specs=[pl.BlockSpec(memory_space=pltpu.VMEM)] + [pl.BlockSpec(memory_space=pltpu.HBM)] * 3,
        out_specs=[pl.BlockSpec(memory_space=pltpu.VMEM)] * 3,
        scratch_shapes=[
            pltpu.VMEM((3, features, rows), jnp.float32),
            pltpu.SemaphoreType.DMA((3,)),
        ],
        compiler_params=pltpu.CompilerParams(vmem_limit_bytes=61 * 2**20),
        name="rounded",
    )(norm_gain[None, :], *masters)


def by_kernels(depth, prompt, *weights):
    g, u, d, both = gather(depth, rounded_by_kernel(*weights), prompt)
    gate_new, up_new, down_new, part = apply(both, g, u, d)
    return gate_new, up_new, down_new, summed(part).T


def by_collectives(prompt, *weights):
    gate_low, up_low, down_low = rounded(*weights)
    whole = lax.all_gather(prompt, "tp", axis=1, tiled=True)
    values = whole.astype(jnp.float32)
    normed = (values * lax.rsqrt(jnp.mean(values * values, axis=1, keepdims=True) + 1e-06)).astype(
        jnp.bfloat16
    )
    contract = (((1,), (1,)), ((), ()))
    gate_new, up_new, down_new = (
        lax.all_gather(gate_low, "fs", axis=1, tiled=True),
        lax.all_gather(up_low, "fs", axis=1, tiled=True),
        lax.all_gather(down_low, "fs", axis=1, tiled=True),
    )
    gate = lax.dot_general(normed, gate_new, contract, preferred_element_type=jnp.float32)
    up = lax.dot_general(normed, up_new, contract, preferred_element_type=jnp.float32)
    hidden = (jax.nn.silu(gate) * up).astype(jnp.bfloat16)
    mixed = lax.psum_scatter(
        lax.dot_general(
            down_new, hidden, (((0,), (1,)), ((), ())), preferred_element_type=jnp.float32
        ),
        "tp",
        scatter_dimension=0,
        tiled=True,
    )
    return (gate_new, up_new, down_new, mixed.astype(jnp.bfloat16))


def solution(mesh):
    placed = (P("fs", "tp"), P("fs"), P("fs", "tp"), P("fs", "tp"), P("fs", "tp"))
    members, pair = mesh.shape["fs"], mesh.shape["tp"]

    def on_device(prompt, norm_gain, *masters):
        aligned = norm_gain.shape[0] % LANES == 0 and masters[0].shape[1] % LANES == 0
        if aligned and pair == 2 and members % 4 == 0 and prompt.shape[0] % 16 == 0:
            return by_kernels(members // 4, prompt, norm_gain, *masters)
        return by_collectives(prompt, norm_gain, *masters)

    return jax.shard_map(
        on_device,
        mesh=mesh,
        in_specs=placed,
        out_specs=(P("tp", None), P("tp", None), P("tp", None), P("tp", "fs")),
        check_vma=False,
    )
```
